256 devices in a mesh: grp: 2 (over y), sp: 16 (over z), tp: 8 (over x, core).
Axes of the slice: x: 4, y: 2, z: 16, core: 2. Of those that a mesh axis runs over, the one named last changes fastest.
The devices are a block of a 4x16x16 slice.
Arguments:
- tokens_in: bfloat16 [12288, 4096], P(('grp', 'sp')), parts along dimension 0, may hold values from -6 to 6
- norm_gain: float32 [4096], replicated, may hold values from 0.1 to 1.9
- window_query: bfloat16 [4096, 1024], P('sp', 'tp'), may hold values from -0.09375 to 0.09375
- window_key: bfloat16 [4096, 512], P('sp', 'tp'), may hold values from -0.09375 to 0.09375
- window_value: bfloat16 [4096, 512], P('sp', 'tp'), may hold values from -0.09375 to 0.09375
- window_query_gain: float32 [64], replicated, may hold values from 0.6 to 16
- window_key_gain: float32 [64], replicated, may hold values from 0.6 to 16
- sink_logit: float32 [16], P('tp'), may hold values from 1 to 6
- dense_query: bfloat16 [4096, 1024], P('sp', 'tp'), may hold values from -0.09375 to 0.09375
- dense_key: bfloat16 [4096, 512], P('sp', 'tp'), may hold values from -0.09375 to 0.09375
- dense_value: bfloat16 [4096, 512], P('sp', 'tp'), may hold values from -0.09375 to 0.09375
- dense_query_gain: float32 [64], replicated, may hold values from 1 to 14
- dense_key_gain: float32 [64], replicated, may hold values from 1 to 14
- window_out: bfloat16 [1024, 4096], P('tp', 'sp'), may hold values from -1.5 to 1.5
- dense_out: bfloat16 [1024, 4096], P('tp', 'sp'), may hold values from -3 to 3
Outputs:
- mixed_out: bfloat16 [12288, 4096], P(('grp', 'sp', 'tp')), parts along dimension 0
The draws below stay inside these ranges and needn't reach their ends.
There are 2 independent parts, one for each index of `grp`. The reference program is written for one: setup_inputs(seed, part) draws one part's arguments, and reference() takes and returns one part's arrays. A program takes and returns all parts, laid end to end along the dimension named above; an argument that names none is the same for every part. Nothing has to cross between parts.
All inputs are finite; a program needn't handle non-finite values.
Results may differ from the reference program's by a relative error of at most 0.03.
The reference program's roundings to bfloat16 on the way count: a program that leaves them out, or rounds other values in their place, can miss the bound.
Values may be sent and summed in bfloat16 or wider, within the bound.
No kernel may reach another device: no remote copies, remote signals or barrier semaphores. Data moves between devices by JAX's collectives and lax.ppermute only.
A program may use at most 64 MiB of HBM per device.

```python
import jax
import jax.numpy as jnp
from jax import lax

D = 4096
B_HEADS = 16
B_KV = 8
C_HEADS = 16
C_KV = 8
HD = 64
WINDOW = 128
GRID_W = 64
TOKENS = 6144
N_TP = 8


def gain_values(key, salt, low, high, hidden_low, hidden_high):
    subkey = jax.random.fold_in(key, salt)
    return jax.random.uniform(subkey, (HD,), jnp.float32, low, high)


def draw_window_query_gain(key, part):
    return gain_values(key, 101, 0.6, 1.6, 12.0, 16.0)


def draw_window_key_gain(key, part):
    return gain_values(key, 102, 0.6, 1.6, 12.0, 16.0)


def draw_dense_query_gain(key, part):
    return gain_values(key, 103, 1.0, 1.8, 10.0, 14.0)


def draw_dense_key_gain(key, part):
    return gain_values(key, 104, 1.0, 1.8, 10.0, 14.0)


def steps_of(key, shape, pieces, least, top_value):
    loudness = 1.0
    for axis_at, blocks in pieces:
        draws = jax.random.uniform(jax.random.fold_in(jax.random.fold_in(key, 6), axis_at), (blocks,), jnp.float32, least / len(pieces), top_value / len(pieces))
        loudness = loudness * jnp.repeat(jnp.exp(draws), shape[axis_at] // blocks).reshape((-1,) + (1,) * (len(shape) - 1 - axis_at))
    return loudness


def noise(key, extent, deviation, reach, cuts=(), held_as=jnp.bfloat16):
    loudness = steps_of(key, extent, cuts, -0.22, 0.18) if cuts else 1.0
    entries = jax.random.normal(key, extent, jnp.float32) * deviation * loudness
    return jnp.minimum(jnp.maximum(entries, -reach), reach).astype(held_as)


def setup_inputs(seed: int = 0, part: int = 0) -> dict:
    seeds = jax.random.split(jax.random.key(seed), 16)
    part_splits = jax.random.split(jax.random.fold_in(seeds[15], part), 16)
    tokens_in = noise(part_splits[0], (TOKENS, D), 1.0, 6.0, ((0, 16),))
    norm_gain = jnp.clip(1.0 + 0.18 * jax.random.normal(seeds[1], (D,), jnp.float32), 0.1, 1.9)
    window_query = noise(seeds[2], (D, B_HEADS * HD), D ** -0.5, 0.09375, ((0, 16), (1, 8)))
    window_key = noise(seeds[3], (D, B_KV * HD), D ** -0.5, 0.09375, ((0, 16), (1, 8)))
    window_value = noise(seeds[4], (D, B_KV * HD), D ** -0.5, 0.09375, ((0, 16), (1, 8)))
    window_query_gain = draw_window_query_gain(jax.random.fold_in(seeds[15], 71), part)
    window_key_gain = draw_window_key_gain(jax.random.fold_in(seeds[15], 71), part)
    sink_logit = jnp.clip(1.0 + 5.0 * jax.random.uniform(seeds[7], (B_HEADS,), jnp.float32) ** steps_of(seeds[7], (B_HEADS,), ((0, 8),), -0.2, 0.2), 1.0, 6.0)
    dense_query = noise(seeds[8], (D, C_HEADS * HD), D ** -0.5, 0.09375, ((0, 16), (1, 8)))
    dense_key = noise(seeds[9], (D, C_KV * HD), D ** -0.5, 0.09375, ((0, 16), (1, 8)))
    dense_value = noise(seeds[10], (D, C_KV * HD), D ** -0.5, 0.09375, ((0, 16), (1, 8)))
    dense_query_gain = draw_dense_query_gain(jax.random.fold_in(seeds[15], 71), part)
    dense_key_gain = draw_dense_key_gain(jax.random.fold_in(seeds[15], 71), part)
    window_out = noise(seeds[13], (B_HEADS * HD, D), 0.25, 1.5, ((0, 8), (1, 16)))
    dense_out = noise(seeds[14], (C_HEADS * HD, D), 0.5, 3.0, ((0, 8), (1, 16)))
    return {"tokens_in": tokens_in, "norm_gain": norm_gain, "window_query": window_query, "window_key": window_key, "window_value": window_value, "window_query_gain": window_query_gain, "window_key_gain": window_key_gain, "sink_logit": sink_logit, "dense_query": dense_query, "dense_key": dense_key, "dense_value": dense_value, "dense_query_gain": dense_query_gain, "dense_key_gain": dense_key_gain, "window_out": window_out, "dense_out": dense_out}


EPS = 1e-06
THETA = 10000.0

def store(values):
    return lax.optimization_barrier(values.astype(jnp.bfloat16))

def rope_table(places, width):
    inverse = THETA ** (-jnp.arange(0, width, 2, dtype=jnp.float32) / width)
    angles = places.astype(jnp.float32)[:, None] * inverse[None, :]
    angles = jnp.concatenate([angles, angles], axis=-1)
    return (jnp.cos(angles), jnp.sin(angles))

def turn(values, tables):
    cosine, sine = tables
    middle = values.shape[-1] // 2
    rotated = jnp.concatenate([-values[..., middle:], values[..., :middle]], axis=-1)
    return values * cosine[:, None, :] + rotated * sine[:, None, :]

def head_norm(projected, gain):
    width = gain.shape[0]
    heads = projected.reshape(projected.shape[0], -1, width)
    return heads * lax.rsqrt(lax.optimization_barrier(jnp.mean(heads * heads, axis=-1, keepdims=True)) + EPS) * gain

def line_heads(projected, gain, places):
    normed = head_norm(projected, gain)
    return turn(normed, rope_table(places, gain.shape[0])).reshape(projected.shape)

def grid_heads(projected, gain, places):
    normed = head_norm(projected, gain)
    middle = gain.shape[0] // 2
    by_row = turn(normed[..., :middle], rope_table(places // GRID_W, middle))
    by_col = turn(normed[..., middle:], rope_table(places % GRID_W, middle))
    return jnp.concatenate([by_row, by_col], axis=-1).reshape(projected.shape)

def banded(query, keys_ext, values_ext, offset, total_len, sink_logit):
    length = query.shape[0]
    kv_heads = keys_ext.shape[1] // HD
    group_size = query.shape[1] // (HD * kv_heads)
    block_count = length // WINDOW
    query_blocks = query.astype(jnp.float32).reshape(block_count, WINDOW, kv_heads, group_size, HD)
    key_blocks = keys_ext.astype(jnp.float32).reshape(block_count + 2, WINDOW, kv_heads, HD)
    value_blocks = values_ext.astype(jnp.float32).reshape(block_count + 2, WINDOW, kv_heads, HD)
    key_near = jnp.concatenate([key_blocks[:-2], key_blocks[1:-1], key_blocks[2:]], axis=1)
    value_near = jnp.concatenate([value_blocks[:-2], value_blocks[1:-1], value_blocks[2:]], axis=1)
    scores = jnp.einsum('nqhgd,nkhd->nhgqk', query_blocks, key_near) * HD ** (-0.5)
    query_pos = offset + jnp.arange(length, dtype=jnp.int32).reshape(block_count, WINDOW)
    key_pos = offset - WINDOW + (jnp.arange(block_count, dtype=jnp.int32)[:, None] * WINDOW + jnp.arange(3 * WINDOW, dtype=jnp.int32)[None, :])
    valid = (jnp.abs(query_pos[:, :, None] - key_pos[:, None, :]) <= WINDOW) & (key_pos >= 0)[:, None, :] & (key_pos < total_len)[:, None, :]
    scores = jnp.where(valid[:, None, None], scores, -jnp.inf)
    floor = sink_logit.reshape(kv_heads, group_size)[None, :, :, None, None]
    top = jnp.maximum(lax.optimization_barrier(jnp.max(scores, axis=-1, keepdims=True)), floor)
    expon = jnp.exp(scores - top)
    weights = store(expon / (lax.optimization_barrier(jnp.sum(expon, axis=-1, keepdims=True)) + jnp.exp(floor - top)))
    result = jnp.einsum('nhgqk,nkhd->nqhgd', weights.astype(jnp.float32), value_near)
    return result.reshape(length, -1)

def dense_attention(query, keys, values):
    length = query.shape[0]
    kv_heads = keys.shape[1] // HD
    group_size = query.shape[1] // (HD * kv_heads)
    if length % 256 == 0:
        block = 256
    elif length % 128 == 0:
        block = 128
    else:
        block = length
    query_blocks = query.astype(jnp.float32).reshape(length // block, block, kv_heads, group_size, HD)
    key_heads = keys.astype(jnp.float32).reshape(length, kv_heads, HD)
    value_heads = values.astype(jnp.float32).reshape(length, kv_heads, HD)

    def one_block(query_block):
        scores = jnp.einsum('qhgd,khd->hgqk', query_block, key_heads) * HD ** (-0.5)
        top = lax.optimization_barrier(jnp.max(scores, axis=-1, keepdims=True))
        expon = jnp.exp(scores - top)
        total = lax.optimization_barrier(jnp.sum(expon, axis=-1))
        rounded = store(expon).astype(jnp.float32)
        summed = jnp.einsum('hgqk,khd->qhgd', rounded, value_heads)
        return summed / jnp.transpose(total, (2, 0, 1))[..., None]
    result = lax.map(one_block, query_blocks)
    return result.reshape(length, -1)

def reference(tokens_in, norm_gain, window_query, window_key, window_value, window_query_gain, window_key_gain, sink_logit, dense_query, dense_key, dense_value, dense_query_gain, dense_key_gain, window_out, dense_out):
    inputs = tokens_in.astype(jnp.float32)
    normed = (inputs * lax.rsqrt(lax.optimization_barrier(jnp.mean(inputs * inputs, axis=-1, keepdims=True)) + EPS) * norm_gain).astype(jnp.bfloat16)

    def project(weight):
        return jnp.dot(normed, weight, preferred_element_type=jnp.float32)
    places = jnp.arange(TOKENS, dtype=jnp.int32)
    query_win = store(line_heads(project(window_query), window_query_gain, places))
    key_win = store(line_heads(project(window_key), window_key_gain, places))
    value_win = store(project(window_value))
    query_den = store(grid_heads(project(dense_query), dense_query_gain, places))
    key_den = store(grid_heads(project(dense_key), dense_key_gain, places))
    value_den = store(project(dense_value))
    margin = ((WINDOW, WINDOW), (0, 0))
    att_win = store(banded(query_win, jnp.pad(key_win, margin), jnp.pad(value_win, margin), 0, TOKENS, sink_logit))
    att_den = store(dense_attention(query_den, key_den, value_den))
    win_parts = att_win.reshape(TOKENS, N_TP, -1).transpose(1, 0, 2)
    den_parts = att_den.reshape(TOKENS, N_TP, -1).transpose(1, 0, 2)
    win_rows = window_out.reshape(N_TP, -1, D)
    den_rows = dense_out.reshape(N_TP, -1, D)

    def add_group(running, members):
        win_part, win_weight, den_part, den_weight = members
        partial_value = jnp.dot(win_part, win_weight, preferred_element_type=jnp.float32) + jnp.dot(den_part, den_weight, preferred_element_type=jnp.float32)
        return (running + store(partial_value).astype(jnp.float32), None)
    running, unused = lax.scan(add_group, jnp.zeros((TOKENS, D), jnp.float32), (win_parts, win_rows, den_parts, den_rows))
    return running.astype(jnp.bfloat16)
```

```python
import functools

import jax
import jax.numpy as jnp
from jax import lax
from jax.experimental import pallas as pl
from jax.experimental.pallas import tpu as pltpu
from jax.sharding import PartitionSpec as P

HD = 64
WINDOW = 128
GRID_W = 64
EPS = 1e-06
THETA = 10000.0
LANES = 2 * HD
F32 = jnp.float32
BF16 = jnp.bfloat16


def dotf(a, b):
    return jnp.dot(a, b, preferred_element_type=F32)


def frequencies(width):
    return THETA ** (-jnp.arange(0, width, 2, dtype=F32) / width)


def packed_angles(places):
    line, grid = frequencies(HD), frequencies(HD // 2)
    inverse = jnp.concatenate([line, grid, grid, jnp.zeros((HD,), F32)])
    lane = lax.broadcasted_iota(jnp.int32, (places.shape[0], LANES), 1)
    t = places[:, None]
    at = jnp.where(lane < HD // 2, t, jnp.where(lane < 3 * HD // 4, t // GRID_W, t % GRID_W))
    return at.astype(F32) * inverse[None, :]


def table_kernel(cosine, sine, cos_w, sin_w, cos_d, sin_d):
    lane = lane_index(cosine.shape[0])
    quarter = HD // 4

    def between(x, low, high):
        return jnp.where((lane >= low) & (lane < high), x, 0.0)

    def line(x):
        x = between(x, 0, 2 * quarter)
        x = x + pltpu.roll(x, 2 * quarter, 1)
        return x + pltpu.roll(x, 4 * quarter, 1)

    def grid(x):
        row = pltpu.roll(between(x, 2 * quarter, 3 * quarter), LANES - 2 * quarter, 1)
        col = pltpu.roll(between(x, 3 * quarter, 4 * quarter), LANES - quarter, 1)
        x = row + col
        x = x + pltpu.roll(x, quarter, 1)
        return x + pltpu.roll(x, 4 * quarter, 1)

    cos_w[...] = line(cosine[...])
    cos_d[...] = grid(cosine[...])
    x = line(sine[...])
    sin_w[...] = jnp.where(lane % HD < HD // 2, -x, x)
    x = grid(sine[...])
    sin_d[...] = jnp.where(lane % (HD // 2) < quarter, -x, x)


def join_kernel(dq, wq, dk, dv, wk, wv, out):
    out[:, 0:LANES] = dq[...]
    out[:, LANES : 2 * LANES] = wq[...]
    pair = jnp.concatenate([dk[...], dv[...]], axis=0).astype(F32)
    out[:, 2 * LANES : 3 * LANES] = pair.T.astype(BF16)
    pair = jnp.concatenate([wk[...], wv[...]], axis=0).astype(F32)
    out[:, 3 * LANES : 4 * LANES] = pair.T.astype(BF16)


def lane_index(rows):
    return lax.broadcasted_iota(jnp.int32, (rows, LANES), 1)


def head_norm(x, lane, gain):
    squares = x * x
    low = jnp.sum(jnp.where(lane < HD, squares, 0.0), axis=-1, keepdims=True)
    high = jnp.sum(jnp.where(lane < HD, 0.0, squares), axis=-1, keepdims=True)
    mean = jnp.where(lane < HD, low, high) * (1.0 / HD)
    return x * lax.rsqrt(mean + EPS) * gain


def turn(x, lane, cosine, sine, half):
    up = pltpu.roll(x, LANES - half, 1)
    down = pltpu.roll(x, half, 1)
    return x * cosine + jnp.where(lane % (2 * half) < half, up, down) * sine


def keyed_values(x, lane, gain, cosine, sine, half):
    return jnp.where(lane < HD, turn(head_norm(x, lane, gain), lane, cosine, sine, half), x).astype(BF16)


def load_kernel(acc, gains, cos_d, sin_d, wo_win, wo_den, load):
    rows = acc.shape[0]
    lane = lane_index(rows)
    high, part = wo_win.shape[0], rows // 2
    kv = keyed_values(acc[...], lane, gains[2:3, :], cos_d[...], sin_d[...], HD // 4)
    load[2 * high : 2 * high + part, 0:LANES] = kv[0:part]
    load[2 * high : 2 * high + part, LANES : 2 * LANES] = kv[part:rows]
    load[0:high, :] = wo_win[...]
    load[high : 2 * high, :] = wo_den[...]


def rest_kernel(core, acc, gains, cos_w, sin_w, cos_d, sin_d, q_den, q_win, kv_win, give, keep):
    rows = acc.shape[0]
    lane = lane_index(rows)

    def put_query(out, col, cosine, sine, half):
        normed = head_norm(acc[:, col * LANES : (col + 1) * LANES], lane, gains[col : col + 1, :])
        turned = turn(normed, lane, cosine[...], sine[...], half)
        out[0:rows, :] = jnp.where(lane < HD, turned, 0.0).astype(BF16)
        out[rows : 2 * rows, :] = jnp.where(lane < HD, pltpu.roll(turned, HD, 1), 0.0).astype(BF16)

    kv = keyed_values(acc[:, 3 * LANES :], lane, gains[3:4, :], cos_w[...], sin_w[...], HD // 2)
    kv_win[...] = kv
    first = core[0] == 0
    head, tail = kv[:WINDOW].astype(F32), kv[rows - WINDOW :].astype(F32)
    give[...] = jnp.where(first, head, tail).astype(BF16)
    keep[...] = jnp.where(first, tail, head).astype(BF16)
    put_query(q_den, 0, cos_d, sin_d, HD // 4)
    put_query(q_win, 1, cos_w, sin_w, HD // 2)


def qkt(q, k):
    return lax.dot_general(q, k, (((1,), (1,)), ((), ())), preferred_element_type=F32)


def join_heads(first, second, lane):
    return jnp.where(lane < HD, pltpu.roll(first, HD, 1), second).astype(BF16)


def window_kernel(place, sinks, q, mine, mid, other, out):
    rows = mid.shape[0]
    first = place[2] == 0
    one, two = mine[0:WINDOW, :].astype(F32), other[...].astype(F32)
    low, high = jnp.where(first, one, two).astype(BF16), jnp.where(first, two, one).astype(BF16)
    ext = jnp.concatenate([low, mid[...], high], axis=0)
    span = 3 * WINDOW
    lane = lane_index(WINDOW)
    row = lax.broadcasted_iota(jnp.int32, (WINDOW, span), 0)
    col = lax.broadcasted_iota(jnp.int32, (WINDOW, span), 1)
    near = (col - row >= 0) & (col - row <= 2 * WINDOW)
    for n in range(rows // WINDOW):
        kv = ext[n * WINDOW : n * WINDOW + span, :]
        key_pos = place[0] + (n - 1) * WINDOW + col
        valid = near & (key_pos >= 0) & (key_pos < place[1])
        done = []
        for h in range(2):
            s = qkt(q[h * rows + n * WINDOW : h * rows + (n + 1) * WINDOW, :], kv) * HD ** (-0.5)
            s = jnp.where(valid, s, -jnp.inf)
            floor = sinks[h]
            top = jnp.maximum(jnp.max(s, axis=-1, keepdims=True), floor)
            e = jnp.exp(s - top)
            weights = e / (jnp.sum(e, axis=-1, keepdims=True) + jnp.exp(floor - top))
            done.append(dotf(weights.astype(BF16), kv))
        out[n * WINDOW : (n + 1) * WINDOW, :] = join_heads(done[0], done[1], lane)


def dense_kernel(first, last, count, *refs):
    q, blocks, rest = refs[0], refs[1 : 1 + count], refs[1 + count :]
    carry, outs = ((), rest) if first else (rest[:2], rest[2:])
    scale = HD ** (-0.5) * 1.4426950408889634
    half = blocks[0].shape[0] - 2 * LANES
    rows = q.shape[0] // 2

    def keys(ref):
        block = ref[ref.shape[0] - half :, :]
        return [block[:, :LANES], block[:, LANES:]]

    for h in range(2):
        at = slice(h * rows, (h + 1) * rows)
        query = q[at, :]
        acc, top = (None, None) if first else (carry[0][at, :], carry[1][at, 0:1])
        for k in range(0, count, 2):
            kv = jnp.concatenate(keys(blocks[k]) + keys(blocks[k + 1]), axis=0)
            wide = lax.broadcasted_iota(jnp.int32, kv.shape, 1)
            values = jnp.where(wide < HD, jnp.ones_like(kv), kv)
            s = qkt(query, kv)
            here = jnp.max(s, axis=-1, keepdims=True)
            new = here if top is None else jnp.maximum(top, here)
            p = jnp.exp2((s - new) * scale).astype(BF16)
            part = dotf(p, values)
            acc = part if top is None else acc * jnp.exp2((top - new) * scale) + part
            top = new
        if last:
            outs[0][at, :] = (acc / pltpu.roll(acc, HD, 1)).astype(BF16)
        else:
            outs[0][at, :] = acc
            outs[1][at, :] = jnp.broadcast_to(top, acc.shape)


def out_kernel(turns, owners, att_win, att_den, *refs):
    blocks, out = refs[:-1], refs[-1]
    parts, share, _ = out.shape
    rows = att_win.shape[0]
    lane = lane_index(share)
    pieces = []
    for r in range(parts):
        at = pl.multiple_of(turns[r] * share, 16)
        low = att_den[pl.ds(at, share), :].astype(F32)
        high = att_den[pl.ds(rows + at, share), :].astype(F32)
        pieces.append(jnp.concatenate([att_win[pl.ds(at, share), :], join_heads(low, high, lane)], axis=1))
    att = jnp.concatenate(pieces, axis=0)
    for i, block in enumerate(blocks):
        width = block.shape[1]
        res = dotf(att, block[0:width, :]).astype(BF16)
        cols = pl.ds(pl.multiple_of(owners[i] * width, width), width)
        for r in range(parts):
            out[r, :, cols] = res[r * share : (r + 1) * share, :]


def run(kernel, outs, args, smem=0, dtype=BF16, **more):
    specs = [pl.BlockSpec(memory_space=pltpu.SMEM)] * smem + [pl.BlockSpec(memory_space=pltpu.VMEM)] * (len(args) - smem)
    return pl.pallas_call(
        kernel,
        out_shape=[jax.ShapeDtypeStruct(s, dtype) for s in outs],
        in_specs=specs,
        **more,
        out_specs=[pl.BlockSpec(memory_space=pltpu.VMEM)] * len(outs),
    )(*args)


def swap(x):
    return lax.ppermute(x, "tp", [(i, i ^ 1) for i in range(lax.axis_size("tp"))])


def step(x):
    n, t = lax.axis_size("sp"), lax.axis_size("tp")
    pairs = [(s * t + c, (s + 1 - 2 * (c % 2)) % n * t + c) for s in range(n) for c in range(t)]
    return lax.ppermute(x, ("sp", "tp"), pairs)


def local(
    tokens_in,
    norm_gain,
    window_query,
    window_key,
    window_value,
    window_query_gain,
    window_key_gain,
    sink_logit,
    dense_query,
    dense_key,
    dense_value,
    dense_query_gain,
    dense_key_gain,
    window_out,
    dense_out,
):
    length = tokens_in.shape[0]
    n = lax.axis_size("sp")
    half = n // 2
    me = lax.axis_index("sp")
    tp = lax.axis_index("tp")
    ntp = lax.axis_size("tp")
    depth = window_query.shape[0]
    way = 1 - 2 * (tp % 2)

    (block,) = run(
        join_kernel,
        [(depth, 4 * LANES)],
        (dense_query, window_query, dense_key.T, dense_value.T, window_key.T, window_value.T),
    )
    inputs = tokens_in.astype(F32)
    normed = (
        inputs * lax.rsqrt(jnp.mean(inputs * inputs, axis=-1, keepdims=True) + EPS) * norm_gain
    ).astype(BF16)

    def product_in(owner, weights):
        return dotf(lax.dynamic_slice_in_dim(normed, (owner % n) * depth, depth, axis=1), weights)

    own = block
    par = swap(block)
    total = product_in(me, block)
    offset = me * length
    for d in range(1, half + 1):
        own = step(own)
        if d < half:
            par = step(par)
            total = total + product_in(me + way * d, swap(par))
        if d == 2:
            offset, own = lax.optimization_barrier((offset, own))
        total = total + product_in(me - way * d, own)

    angles = packed_angles(offset + jnp.arange(length, dtype=jnp.int32))
    cos_w, sin_w, cos_d, sin_d = run(
        table_kernel, [(length, LANES)] * 4, (jnp.cos(angles), jnp.sin(angles)), dtype=F32
    )
    gains = jnp.stack(
        [jnp.tile(g, 2) for g in (dense_query_gain, window_query_gain, dense_key_gain, window_key_gain)]
    )
    wide = window_out.shape[1]
    load_rows = 2 * window_out.shape[0] + length // 2
    args = (total, gains, cos_d, sin_d, window_out, dense_out)
    load = pl.pallas_call(
        load_kernel,
        grid=(1,),
        out_shape=jax.ShapeDtypeStruct((load_rows, wide), BF16),
        in_specs=[pl.BlockSpec((length, LANES), lambda i: (0, 2))]
        + [pl.BlockSpec(a.shape, lambda i: (0, 0)) for a in args[1:]],
        out_specs=pl.BlockSpec((load_rows, wide), lambda i: (0, 0)),
    )(*args)
    core_here = (tp % 2).astype(jnp.int32)
    pieces = [(2 * length, LANES)] * 2 + [(length, LANES)] + [(WINDOW, LANES)] * 2
    q_den, q_win, kv_win, give, keep = run(
        rest_kernel, pieces, (core_here.reshape(1), total, gains, cos_w, sin_w, cos_d, sin_d), smem=1
    )
    place = jnp.stack([offset, length * n, core_here]).astype(jnp.int32)
    edges = step(jnp.concatenate([keep, swap(give)], axis=0))
    far_edge = swap(edges[WINDOW:])

    def dense(blocks, carry, last):
        shape = jax.ShapeDtypeStruct((2 * length, LANES), BF16 if last else F32)
        args = (q_den, *blocks, *carry)
        return pl.pallas_call(
            functools.partial(dense_kernel, not carry, last, len(blocks)),
            out_shape=[shape] if last else [shape, shape],
            in_specs=[pl.BlockSpec(memory_space=pltpu.VMEM)] * len(args),
            out_specs=[pl.BlockSpec(memory_space=pltpu.VMEM)] * (1 if last else 2),
        )(*args)

    own, par = load, swap(load)
    every, owners, carry, used = [load], [me], (), 0
    for d in range(1, half + 1):
        if d == 5:
            (att_win,) = run(
                window_kernel, [(length, LANES)], (place, sink_logit, q_win, edges, kv_win, far_edge), smem=2
            )
            own, att_win = lax.optimization_barrier((own, att_win))
        if d >= 4 and d % 2 == 0:
            own, carry = lax.optimization_barrier((own, carry))
        own = step(own)
        every.append(own)
        owners.append(me - way * d)
        if d < half:
            par = step(par)
            every.append(swap(par))
            owners.append(me + way * d)
        while len(every) - used >= 4 and d < half:
            carry = dense(every[used : used + 4], carry, False)
            used += 4
    (att_den,) = dense(every[used:], carry, True)
    owners = jnp.stack(owners).astype(jnp.int32) % n
    places_out = every
    core, x = tp % 2, tp // 2
    nx = ntp // 2
    share = length // ntp

    def product(which):
        turns = jnp.stack([((x + r) % nx) * 2 + which for r in range(nx)]).astype(jnp.int32)
        (res,) = run(
            out_kernel, [(nx, share, wide * n)], (turns, owners, att_win, att_den, *places_out), smem=2
        )
        return res

    given = lax.ppermute(product(1 - core), "tp", [(i, i ^ 1) for i in range(ntp)])
    kept = product(core)
    sums = [kept[r].astype(F32) + given[r].astype(F32) for r in range(nx)]
    got = {}
    for r in sorted(range(1, nx), key=lambda r: -min(r, nx - r)):
        got[r] = lax.ppermute(sums[r].astype(BF16), "tp", [(i, (i + 2 * r) % ntp) for i in range(ntp)])
    out = sums[0]
    for r in range(1, nx):
        out = out + got[r].astype(F32)
    return out.astype(BF16)


def solution(mesh):
    return jax.shard_map(
        local,
        mesh=mesh,
        in_specs=(
            P(("grp", "sp"), None),
            P(),
            P("sp", "tp"),
            P("sp", "tp"),
            P("sp", "tp"),
            P(),
            P(),
            P("tp"),
            P("sp", "tp"),
            P("sp", "tp"),
            P("sp", "tp"),
            P(),
            P(),
            P("tp", "sp"),
            P("tp", "sp"),
        ),
        out_specs=P(("grp", "sp", "tp"), None),
        check_vma=False,
    )
```

```python
import functools

import jax
import jax.numpy as jnp
from jax import lax
from jax.experimental import pallas as pl
from jax.experimental.pallas import tpu as pltpu
from jax.sharding import PartitionSpec as P

HD = 64
WINDOW = 128
GRID_W = 64
EPS = 1e-06
THETA = 10000.0
LANES = 2 * HD
F32 = jnp.float32
BF16 = jnp.bfloat16


def dotf(a, b):
    return jnp.dot(a, b, preferred_element_type=F32)


def frequencies(width):
    return THETA ** (-jnp.arange(0, width, 2, dtype=F32) / width)


def packed_angles(places):
    line, grid = frequencies(HD), frequencies(HD // 2)
    inverse = jnp.concatenate([line, grid, grid, jnp.zeros((HD,), F32)])
    lane = lax.broadcasted_iota(jnp.int32, (places.shape[0], LANES), 1)
    t = places[:, None]
    at = jnp.where(lane < HD // 2, t, jnp.where(lane < 3 * HD // 4, t // GRID_W, t % GRID_W))
    return at.astype(F32) * inverse[None, :]


def table_kernel(cosine, sine, cos_w, sin_w, cos_d, sin_d):
    lane = lane_index(cosine.shape[0])
    quarter = HD // 4

    def between(x, low, high):
        return jnp.where((lane >= low) & (lane < high), x, 0.0)

    def line(x):
        x = between(x, 0, 2 * quarter)
        x = x + pltpu.roll(x, 2 * quarter, 1)
        return x + pltpu.roll(x, 4 * quarter, 1)

    def grid(x):
        row = pltpu.roll(between(x, 2 * quarter, 3 * quarter), LANES - 2 * quarter, 1)
        col = pltpu.roll(between(x, 3 * quarter, 4 * quarter), LANES - quarter, 1)
        x = row + col
        x = x + pltpu.roll(x, quarter, 1)
        return x + pltpu.roll(x, 4 * quarter, 1)

    cos_w[...] = line(cosine[...])
    cos_d[...] = grid(cosine[...])
    x = line(sine[...])
    sin_w[...] = jnp.where(lane % HD < HD // 2, -x, x)
    x = grid(sine[...])
    sin_d[...] = jnp.where(lane % (HD // 2) < quarter, -x, x)


def join_kernel(dq, wq, dk, dv, wk, wv, out):
    out[:, 0:LANES] = dq[...]
    out[:, LANES : 2 * LANES] = wq[...]
    pair = jnp.concatenate([dk[...], dv[...]], axis=0).astype(F32)
    out[:, 2 * LANES : 3 * LANES] = pair.T.astype(BF16)
    pair = jnp.concatenate([wk[...], wv[...]], axis=0).astype(F32)
    out[:, 3 * LANES : 4 * LANES] = pair.T.astype(BF16)


def lane_index(rows):
    return lax.broadcasted_iota(jnp.int32, (rows, LANES), 1)


def head_norm(x, lane, gain):
    squares = x * x
    low = jnp.sum(jnp.where(lane < HD, squares, 0.0), axis=-1, keepdims=True)
    high = jnp.sum(jnp.where(lane < HD, 0.0, squares), axis=-1, keepdims=True)
    mean = jnp.where(lane < HD, low, high) * (1.0 / HD)
    return x * lax.rsqrt(mean + EPS) * gain


def turn(x, lane, cosine, sine, half):
    up = pltpu.roll(x, LANES - half, 1)
    down = pltpu.roll(x, half, 1)
    return x * cosine + jnp.where(lane % (2 * half) < half, up, down) * sine


def keyed_values(x, lane, gain, cosine, sine, half):
    return jnp.where(lane < HD, turn(head_norm(x, lane, gain), lane, cosine, sine, half), x).astype(BF16)


def load_kernel(acc, gains, cos_d, sin_d, wo_win, wo_den, load):
    rows = acc.shape[0]
    lane = lane_index(rows)
    high, part = wo_win.shape[0], rows // 2
    kv = keyed_values(acc[...], lane, gains[2:3, :], cos_d[...], sin_d[...], HD // 4)
    load[2 * high : 2 * high + part, 0:LANES] = kv[0:part]
    load[2 * high : 2 * high + part, LANES : 2 * LANES] = kv[part:rows]
    load[0:high, :] = wo_win[...]
    load[high : 2 * high, :] = wo_den[...]


def rest_kernel(core, acc, gains, cos_w, sin_w, cos_d, sin_d, q_den, q_win, kv_win, give, keep):
    rows = acc.shape[0]
    lane = lane_index(rows)

    def put_query(out, col, cosine, sine, half):
        normed = head_norm(acc[:, col * LANES : (col + 1) * LANES], lane, gains[col : col + 1, :])
        turned = turn(normed, lane, cosine[...], sine[...], half)
        out[0:rows, :] = jnp.where(lane < HD, turned, 0.0).astype(BF16)
        out[rows : 2 * rows, :] = jnp.where(lane < HD, pltpu.roll(turned, HD, 1), 0.0).astype(BF16)

    kv = keyed_values(acc[:, 3 * LANES :], lane, gains[3:4, :], cos_w[...], sin_w[...], HD // 2)
    kv_win[...] = kv
    first = core[0] == 0
    head, tail = kv[:WINDOW].astype(F32), kv[rows - WINDOW :].astype(F32)
    give[...] = jnp.where(first, head, tail).astype(BF16)
    keep[...] = jnp.where(first, tail, head).astype(BF16)
    put_query(q_den, 0, cos_d, sin_d, HD // 4)
    put_query(q_win, 1, cos_w, sin_w, HD // 2)


def qkt(q, k):
    return lax.dot_general(q, k, (((1,), (1,)), ((), ())), preferred_element_type=F32)


def join_heads(first, second, lane):
    return jnp.where(lane < HD, pltpu.roll(first, HD, 1), second).astype(BF16)


def window_kernel(place, sinks, q, mine, mid, other, out):
    rows = mid.shape[0]
    first = place[2] == 0
    one, two = mine[0:WINDOW, :].astype(F32), other[...].astype(F32)
    low, high = jnp.where(first, one, two).astype(BF16), jnp.where(first, two, one).astype(BF16)
    ext = jnp.concatenate([low, mid[...], high], axis=0)
    span = 3 * WINDOW
    lane = lane_index(WINDOW)
    row = lax.broadcasted_iota(jnp.int32, (WINDOW, span), 0)
    col = lax.broadcasted_iota(jnp.int32, (WINDOW, span), 1)
    near = (col - row >= 0) & (col - row <= 2 * WINDOW)
    for n in range(rows // WINDOW):
        kv = ext[n * WINDOW : n * WINDOW + span, :]
        key_pos = place[0] + (n - 1) * WINDOW + col
        valid = near & (key_pos >= 0) & (key_pos < place[1])
        done = []
        for h in range(2):
            s = qkt(q[h * rows + n * WINDOW : h * rows + (n + 1) * WINDOW, :], kv) * HD ** (-0.5)
            s = jnp.where(valid, s, -jnp.inf)
            floor = sinks[h]
            top = jnp.maximum(jnp.max(s, axis=-1, keepdims=True), floor)
            e = jnp.exp(s - top)
            weights = e / (jnp.sum(e, axis=-1, keepdims=True) + jnp.exp(floor - top))
            done.append(dotf(weights.astype(BF16), kv))
        out[n * WINDOW : (n + 1) * WINDOW, :] = join_heads(done[0], done[1], lane)


def dense_kernel(first, last, count, *refs):
    q, blocks, rest = refs[0], refs[1 : 1 + count], refs[1 + count :]
    carry, outs = ((), rest) if first else (rest[:2], rest[2:])
    scale = HD ** (-0.5) * 1.4426950408889634
    half = blocks[0].shape[0] - 2 * LANES
    rows = q.shape[0] // 2

    def keys(ref):
        block = ref[ref.shape[0] - half :, :]
        return [block[:, :LANES], block[:, LANES:]]

    for h in range(2):
        at = slice(h * rows, (h + 1) * rows)
        query = q[at, :]
        acc, top = (None, None) if first else (carry[0][at, :], carry[1][at, 0:1])
        for k in range(0, count, 2):
            kv = jnp.concatenate(keys(blocks[k]) + keys(blocks[k + 1]), axis=0)
            wide = lax.broadcasted_iota(jnp.int32, kv.shape, 1)
            values = jnp.where(wide < HD, jnp.ones_like(kv), kv)
            s = qkt(query, kv)
            here = jnp.max(s, axis=-1, keepdims=True)
            new = here if top is None else jnp.maximum(top, here)
            p = jnp.exp2((s - new) * scale).astype(BF16)
            part = dotf(p, values)
            acc = part if top is None else acc * jnp.exp2((top - new) * scale) + part
            top = new
        if last:
            outs[0][at, :] = (acc / pltpu.roll(acc, HD, 1)).astype(BF16)
        else:
            outs[0][at, :] = acc
            outs[1][at, :] = jnp.broadcast_to(top, acc.shape)


def out_kernel(turns, owners, att_win, att_den, *refs):
    blocks, out = refs[:-1], refs[-1]
    parts, share, _ = out.shape
    rows = att_win.shape[0]
    lane = lane_index(share)
    pieces = []
    for r in range(parts):
        at = pl.multiple_of(turns[r] * share, 16)
        low = att_den[pl.ds(at, share), :].astype(F32)
        high = att_den[pl.ds(rows + at, share), :].astype(F32)
        pieces.append(jnp.concatenate([att_win[pl.ds(at, share), :], join_heads(low, high, lane)], axis=1))
    att = jnp.concatenate(pieces, axis=0)
    for i, block in enumerate(blocks):
        width = block.shape[1]
        res = dotf(att, block[0:width, :]).astype(BF16)
        cols = pl.ds(pl.multiple_of(owners[i] * width, width), width)
        for r in range(parts):
            out[r, :, cols] = res[r * share : (r + 1) * share, :]


def run(kernel, outs, args, smem=0, dtype=BF16, **more):
    specs = [pl.BlockSpec(memory_space=pltpu.SMEM)] * smem + [pl.BlockSpec(memory_space=pltpu.VMEM)] * (len(args) - smem)
    return pl.pallas_call(
        kernel,
        out_shape=[jax.ShapeDtypeStruct(s, dtype) for s in outs],
        in_specs=specs,
        **more,
        out_specs=[pl.BlockSpec(memory_space=pltpu.VMEM)] * len(outs),
    )(*args)


def swap(x):
    return lax.ppermute(x, "tp", [(i, i ^ 1) for i in range(lax.axis_size("tp"))])


def step(x):
    n, t = lax.axis_size("sp"), lax.axis_size("tp")
    pairs = [(s * t + c, (s + 1 - 2 * (c % 2)) % n * t + c) for s in range(n) for c in range(t)]
    return lax.ppermute(x, ("sp", "tp"), pairs)


def local(
    tokens_in,
    norm_gain,
    window_query,
    window_key,
    window_value,
    window_query_gain,
    window_key_gain,
    sink_logit,
    dense_query,
    dense_key,
    dense_value,
    dense_query_gain,
    dense_key_gain,
    window_out,
    dense_out,
):
    length = tokens_in.shape[0]
    n = lax.axis_size("sp")
    half = n // 2
    me = lax.axis_index("sp")
    tp = lax.axis_index("tp")
    ntp = lax.axis_size("tp")
    depth = window_query.shape[0]
    way = 1 - 2 * (tp % 2)

    (block,) = run(
        join_kernel,
        [(depth, 4 * LANES)],
        (dense_query, window_query, dense_key.T, dense_value.T, window_key.T, window_value.T),
    )
    inputs = tokens_in.astype(F32)
    inverse = lax.rsqrt(jnp.mean(inputs * inputs, axis=-1, keepdims=True) + EPS)

    def product_in(owner, weights):
        return dotf(lax.dynamic_slice_in_dim(normed, (owner % n) * depth, depth, axis=1), weights)

    own = block
    par = swap(block)
    offset = me * length
    for d in range(1, half + 1):
        own = step(own)
        if d < half:
            par = step(par)
            if d == 1:
                inverse, par = lax.optimization_barrier((inverse, par))
                normed = (inputs * inverse * norm_gain).astype(BF16)
                total = product_in(me, block)
            total = total + product_in(me + way * d, swap(par))
        if d == 4:
            offset, own = lax.optimization_barrier((offset, own))
        total = total + product_in(me - way * d, own)

    angles = packed_angles(offset + jnp.arange(length, dtype=jnp.int32))
    cos_w, sin_w, cos_d, sin_d = run(
        table_kernel, [(length, LANES)] * 4, (jnp.cos(angles), jnp.sin(angles)), dtype=F32
    )
    gains = jnp.stack(
        [jnp.tile(g, 2) for g in (dense_query_gain, window_query_gain, dense_key_gain, window_key_gain)]
    )
    wide = window_out.shape[1]
    load_rows = 2 * window_out.shape[0] + length // 2
    args = (total, gains, cos_d, sin_d, window_out, dense_out)
    load = pl.pallas_call(
        load_kernel,
        grid=(1,),
        out_shape=jax.ShapeDtypeStruct((load_rows, wide), BF16),
        in_specs=[pl.BlockSpec((length, LANES), lambda i: (0, 2))]
        + [pl.BlockSpec(a.shape, lambda i: (0, 0)) for a in args[1:]],
        out_specs=pl.BlockSpec((load_rows, wide), lambda i: (0, 0)),
    )(*args)
    core_here = (tp % 2).astype(jnp.int32)
    pieces = [(2 * length, LANES)] * 2 + [(length, LANES)] + [(WINDOW, LANES)] * 2
    q_den, q_win, kv_win, give, keep = run(
        rest_kernel, pieces, (core_here.reshape(1), total, gains, cos_w, sin_w, cos_d, sin_d), smem=1
    )
    place = jnp.stack([offset, length * n, core_here]).astype(jnp.int32)
    def dense(blocks, carry, last):
        shape = jax.ShapeDtypeStruct((2 * length, LANES), BF16 if last else F32)
        args = (q_den, *blocks, *carry)
        return pl.pallas_call(
            functools.partial(dense_kernel, not carry, last, len(blocks)),
            out_shape=[shape] if last else [shape, shape],
            in_specs=[pl.BlockSpec(memory_space=pltpu.VMEM)] * len(args),
            out_specs=[pl.BlockSpec(memory_space=pltpu.VMEM)] * (1 if last else 2),
        )(*args)

    own, par = load, swap(load)
    every, owners, carry, used = [load], [me], (), 0
    for d in range(1, half + 1):
        if d == 2:
            own, give, keep, kv_win, q_den, q_win = lax.optimization_barrier((own, give, keep, kv_win, q_den, q_win))
            passed = swap(give)
        if d == 3:
            own, passed = lax.optimization_barrier((own, passed))
            edges = step(jnp.concatenate([keep, passed], axis=0))
        if d == 5:
            own, edges = lax.optimization_barrier((own, edges))
            far_edge = swap(edges[WINDOW:])
        if d == 7:
            (att_win,) = run(
                window_kernel, [(length, LANES)], (place, sink_logit, q_win, edges, kv_win, far_edge), smem=2
            )
            own, att_win = lax.optimization_barrier((own, att_win))
        if d >= 4 and d % 2 == 0:
            own, carry = lax.optimization_barrier((own, carry))
        own = step(own)
        every.append(own)
        owners.append(me - way * d)
        if d < half:
            par = step(par)
            every.append(swap(par))
            owners.append(me + way * d)
        while len(every) - used >= 4 and d < half:
            carry = dense(every[used : used + 4], carry, False)
            used += 4
    (att_den,) = dense(every[used:], carry, True)
    owners = jnp.stack(owners).astype(jnp.int32) % n
    places_out = every
    core, x = tp % 2, tp // 2
    nx = ntp // 2
    share = length // ntp

    def product(which):
        turns = jnp.stack([((x + r) % nx) * 2 + which for r in range(nx)]).astype(jnp.int32)
        (res,) = run(
            out_kernel, [(nx, share, wide * n)], (turns, owners, att_win, att_den, *places_out), smem=2
        )
        return res

    given = lax.ppermute(product(1 - core), "tp", [(i, i ^ 1) for i in range(ntp)])
    kept = product(core)
    sums = [kept[r].astype(F32) + given[r].astype(F32) for r in range(nx)]
    got = {}
    for r in sorted(range(1, nx), key=lambda r: -min(r, nx - r)):
        got[r] = lax.ppermute(sums[r].astype(BF16), "tp", [(i, (i + 2 * r) % ntp) for i in range(ntp)])
    out = sums[0]
    for r in range(1, nx):
        out = out + got[r].astype(F32)
    return out.astype(BF16)


def solution(mesh):
    return jax.shard_map(
        local,
        mesh=mesh,
        in_specs=(
            P(("grp", "sp"), None),
            P(),
            P("sp", "tp"),
            P("sp", "tp"),
            P("sp", "tp"),
            P(),
            P(),
            P("tp"),
            P("sp", "tp"),
            P("sp", "tp"),
            P("sp", "tp"),
            P(),
            P(),
            P("tp", "sp"),
            P("tp", "sp"),
        ),
        out_specs=P(("grp", "sp", "tp"), None),
        check_vma=False,
    )
```

```python
import functools

import jax
import jax.numpy as jnp
from jax import lax
from jax.experimental import pallas as pl
from jax.experimental.pallas import tpu as pltpu
from jax.sharding import PartitionSpec as P

HD = 64
WINDOW = 128
GRID_W = 64
EPS = 1e-06
THETA = 10000.0
LANES = 2 * HD
F32 = jnp.float32
BF16 = jnp.bfloat16


def dotf(a, b):
    return jnp.dot(a, b, preferred_element_type=F32)


def frequencies(width):
    return THETA ** (-jnp.arange(0, width, 2, dtype=F32) / width)


def packed_angles(places):
    line, grid = frequencies(HD), frequencies(HD // 2)
    inverse = jnp.concatenate([line, grid, grid, jnp.zeros((HD,), F32)])
    lane = lax.broadcasted_iota(jnp.int32, (places.shape[0], LANES), 1)
    t = places[:, None]
    at = jnp.where(lane < HD // 2, t, jnp.where(lane < 3 * HD // 4, t // GRID_W, t % GRID_W))
    return at.astype(F32) * inverse[None, :]


def table_kernel(cosine, sine, cos_w, sin_w, cos_d, sin_d):
    lane = lane_index(cosine.shape[0])
    quarter = HD // 4

    def between(x, low, high):
        return jnp.where((lane >= low) & (lane < high), x, 0.0)

    def line(x):
        x = between(x, 0, 2 * quarter)
        x = x + pltpu.roll(x, 2 * quarter, 1)
        return x + pltpu.roll(x, 4 * quarter, 1)

    def grid(x):
        row = pltpu.roll(between(x, 2 * quarter, 3 * quarter), LANES - 2 * quarter, 1)
        col = pltpu.roll(between(x, 3 * quarter, 4 * quarter), LANES - quarter, 1)
        x = row + col
        x = x + pltpu.roll(x, quarter, 1)
        return x + pltpu.roll(x, 4 * quarter, 1)

    cos_w[...] = line(cosine[...])
    cos_d[...] = grid(cosine[...])
    x = line(sine[...])
    sin_w[...] = jnp.where(lane % HD < HD // 2, -x, x)
    x = grid(sine[...])
    sin_d[...] = jnp.where(lane % (HD // 2) < quarter, -x, x)


def join_kernel(dq, wq, dk, dv, wk, wv, out):
    out[:, 0:LANES] = dq[...]
    out[:, LANES : 2 * LANES] = wq[...]
    pair = jnp.concatenate([dk[...], dv[...]], axis=0).astype(F32)
    out[:, 2 * LANES : 3 * LANES] = pair.T.astype(BF16)
    pair = jnp.concatenate([wk[...], wv[...]], axis=0).astype(F32)
    out[:, 3 * LANES : 4 * LANES] = pair.T.astype(BF16)


def lane_index(rows):
    return lax.broadcasted_iota(jnp.int32, (rows, LANES), 1)


def head_norm(x, lane, gain):
    squares = x * x
    low = jnp.sum(jnp.where(lane < HD, squares, 0.0), axis=-1, keepdims=True)
    high = jnp.sum(jnp.where(lane < HD, 0.0, squares), axis=-1, keepdims=True)
    mean = jnp.where(lane < HD, low, high) * (1.0 / HD)
    return x * lax.rsqrt(mean + EPS) * gain


def turn(x, lane, cosine, sine, half):
    up = pltpu.roll(x, LANES - half, 1)
    down = pltpu.roll(x, half, 1)
    return x * cosine + jnp.where(lane % (2 * half) < half, up, down) * sine


def keyed_values(x, lane, gain, cosine, sine, half):
    return jnp.where(lane < HD, turn(head_norm(x, lane, gain), lane, cosine, sine, half), x).astype(BF16)


def load_kernel(acc, gains, cos_d, sin_d, wo_win, wo_den, load):
    rows = acc.shape[0]
    lane = lane_index(rows)
    high, part = wo_win.shape[0], rows // 2
    kv = keyed_values(acc[...], lane, gains[2:3, :], cos_d[...], sin_d[...], HD // 4)
    load[2 * high : 2 * high + part, 0:LANES] = kv[0:part]
    load[2 * high : 2 * high + part, LANES : 2 * LANES] = kv[part:rows]
    load[0:high, :] = wo_win[...]
    load[high : 2 * high, :] = wo_den[...]


def rest_kernel(core, acc, gains, cos_w, sin_w, cos_d, sin_d, q_den, q_win, kv_win, give, keep):
    rows = acc.shape[0]
    lane = lane_index(rows)

    def put_query(out, col, cosine, sine, half):
        normed = head_norm(acc[:, col * LANES : (col + 1) * LANES], lane, gains[col : col + 1, :])
        turned = turn(normed, lane, cosine[...], sine[...], half)
        out[0:rows, :] = jnp.where(lane < HD, turned, 0.0).astype(BF16)
        out[rows : 2 * rows, :] = jnp.where(lane < HD, pltpu.roll(turned, HD, 1), 0.0).astype(BF16)

    kv = keyed_values(acc[:, 3 * LANES :], lane, gains[3:4, :], cos_w[...], sin_w[...], HD // 2)
    kv_win[...] = kv
    first = core[0] == 0
    head, tail = kv[:WINDOW].astype(F32), kv[rows - WINDOW :].astype(F32)
    give[...] = jnp.where(first, head, tail).astype(BF16)
    keep[...] = jnp.where(first, tail, head).astype(BF16)
    put_query(q_den, 0, cos_d, sin_d, HD // 4)
    put_query(q_win, 1, cos_w, sin_w, HD // 2)


def qkt(q, k):
    return lax.dot_general(q, k, (((1,), (1,)), ((), ())), preferred_element_type=F32)


def join_heads(first, second, lane):
    return jnp.where(lane < HD, pltpu.roll(first, HD, 1), second).astype(BF16)


def window_kernel(place, sinks, q, mine, mid, other, out):
    rows = mid.shape[0]
    first = place[2] == 0
    one, two = mine[0:WINDOW, :].astype(F32), other[...].astype(F32)
    low, high = jnp.where(first, one, two).astype(BF16), jnp.where(first, two, one).astype(BF16)
    ext = jnp.concatenate([low, mid[...], high], axis=0)
    span = 3 * WINDOW
    lane = lane_index(WINDOW)
    row = lax.broadcasted_iota(jnp.int32, (WINDOW, span), 0)
    col = lax.broadcasted_iota(jnp.int32, (WINDOW, span), 1)
    near = (col - row >= 0) & (col - row <= 2 * WINDOW)
    scores, valid, floor, near_kv = [], [], [], []
    for n in range(rows // WINDOW):
        kv = ext[n * WINDOW : n * WINDOW + span, :]
        near_kv.append(kv)
        key_pos = place[0] + (n - 1) * WINDOW + col
        for h in range(2):
            scores.append(qkt(q[h * rows + n * WINDOW : h * rows + (n + 1) * WINDOW, :], kv))
            valid.append(near & (key_pos >= 0) & (key_pos < place[1]))
            floor.append(jnp.full((WINDOW, 1), sinks[h], F32))
    floor = jnp.concatenate(floor, axis=0)
    s = jnp.concatenate([jnp.where(v, x * HD ** (-0.5), -jnp.inf) for v, x in zip(valid, scores)], axis=0)
    top = jnp.maximum(jnp.max(s, axis=-1, keepdims=True), floor)
    e = jnp.exp(s - top)
    weights = e / (jnp.sum(e, axis=-1, keepdims=True) + jnp.exp(floor - top))
    weights = weights.astype(BF16)
    for n, kv in enumerate(near_kv):
        base = 2 * n * WINDOW
        first_head = dotf(weights[base : base + WINDOW], kv)
        second_head = dotf(weights[base + WINDOW : base + 2 * WINDOW], kv)
        out[n * WINDOW : (n + 1) * WINDOW, :] = join_heads(first_head, second_head, lane)


def dense_kernel(first, last, count, *refs):
    q, blocks, rest = refs[0], refs[1 : 1 + count], refs[1 + count :]
    carry, outs = ((), rest) if first else (rest[:2], rest[2:])
    scale = HD ** (-0.5) * 1.4426950408889634
    half = blocks[0].shape[0] - 2 * LANES
    rows = q.shape[0] // 2

    def keys(ref):
        block = ref[ref.shape[0] - half :, :]
        return [block[:, :LANES], block[:, LANES:]]

    for h in range(2):
        at = slice(h * rows, (h + 1) * rows)
        query = q[at, :]
        acc, top = (None, None) if first else (carry[0][at, :], carry[1][at, 0:1])
        for k in range(0, count, 4):
            kv = jnp.concatenate([x for ref in blocks[k : k + 4] for x in keys(ref)], axis=0)
            wide = lax.broadcasted_iota(jnp.int32, kv.shape, 1)
            values = jnp.where(wide < HD, jnp.ones_like(kv), kv)
            s = qkt(query, kv)
            here = jnp.max(s, axis=-1, keepdims=True)
            new = here if top is None else jnp.maximum(top, here)
            p = jnp.exp2((s - new) * scale).astype(BF16)
            part = dotf(p, values)
            acc = part if top is None else acc * jnp.exp2((top - new) * scale) + part
            top = new
        if last:
            outs[0][at, :] = (acc / pltpu.roll(acc, HD, 1)).astype(BF16)
        else:
            outs[0][at, :] = acc
            outs[1][at, :] = jnp.broadcast_to(top, acc.shape)


def out_kernel(turns, owners, att_win, att_den, *refs):
    blocks, out = refs[:-1], refs[-1]
    parts, share, _ = out.shape
    rows = att_win.shape[0]
    lane = lane_index(share)
    pieces = []
    for r in range(parts):
        at = pl.multiple_of(turns[r] * share, 16)
        low = att_den[pl.ds(at, share), :].astype(F32)
        high = att_den[pl.ds(rows + at, share), :].astype(F32)
        pieces.append(jnp.concatenate([att_win[pl.ds(at, share), :], join_heads(low, high, lane)], axis=1))
    att = jnp.concatenate(pieces, axis=0)
    for i, block in enumerate(blocks):
        width = block.shape[1]
        res = dotf(att, block[0:width, :]).astype(BF16)
        cols = pl.ds(pl.multiple_of(owners[i] * width, width), width)
        for r in range(parts):
            out[r, :, cols] = res[r * share : (r + 1) * share, :]


def run(kernel, outs, args, smem=0, dtype=BF16, **more):
    specs = [pl.BlockSpec(memory_space=pltpu.SMEM)] * smem + [pl.BlockSpec(memory_space=pltpu.VMEM)] * (len(args) - smem)
    return pl.pallas_call(
        kernel,
        out_shape=[jax.ShapeDtypeStruct(s, dtype) for s in outs],
        in_specs=specs,
        **more,
        out_specs=[pl.BlockSpec(memory_space=pltpu.VMEM)] * len(outs),
    )(*args)


def swap(x):
    return lax.ppermute(x, "tp", [(i, i ^ 1) for i in range(lax.axis_size("tp"))])


def step(x):
    n, t = lax.axis_size("sp"), lax.axis_size("tp")
    pairs = [(s * t + c, (s + 1 - 2 * (c % 2)) % n * t + c) for s in range(n) for c in range(t)]
    return lax.ppermute(x, ("sp", "tp"), pairs)


def local(
    tokens_in,
    norm_gain,
    window_query,
    window_key,
    window_value,
    window_query_gain,
    window_key_gain,
    sink_logit,
    dense_query,
    dense_key,
    dense_value,
    dense_query_gain,
    dense_key_gain,
    window_out,
    dense_out,
):
    length = tokens_in.shape[0]
    n = lax.axis_size("sp")
    half = n // 2
    me = lax.axis_index("sp")
    tp = lax.axis_index("tp")
    ntp = lax.axis_size("tp")
    depth = window_query.shape[0]
    way = 1 - 2 * (tp % 2)

    (block,) = run(
        join_kernel,
        [(depth, 4 * LANES)],
        (dense_query, window_query, dense_key.T, dense_value.T, window_key.T, window_value.T),
    )
    inputs = tokens_in.astype(F32)
    inverse = lax.rsqrt(jnp.mean(inputs * inputs, axis=-1, keepdims=True) + EPS)

    def product_in(owner, weights):
        return dotf(lax.dynamic_slice_in_dim(normed, (owner % n) * depth, depth, axis=1), weights)

    own = block
    par = swap(block)
    offset = me * length
    for d in range(1, half + 1):
        own = step(own)
        if d < half:
            par = step(par)
            if d == 1:
                inverse, par = lax.optimization_barrier((inverse, par))
                normed = (inputs * inverse * norm_gain).astype(BF16)
                total = product_in(me, block)
            total = total + product_in(me + way * d, swap(par))
        if d == 4:
            offset, own = lax.optimization_barrier((offset, own))
        total = total + product_in(me - way * d, own)

    angles = packed_angles(offset + jnp.arange(length, dtype=jnp.int32))
    cos_w, sin_w, cos_d, sin_d = run(
        table_kernel, [(length, LANES)] * 4, (jnp.cos(angles), jnp.sin(angles)), dtype=F32
    )
    gains = jnp.stack(
        [jnp.tile(g, 2) for g in (dense_query_gain, window_query_gain, dense_key_gain, window_key_gain)]
    )
    wide = window_out.shape[1]
    load_rows = 2 * window_out.shape[0] + length // 2
    args = (total, gains, cos_d, sin_d, window_out, dense_out)
    load = pl.pallas_call(
        load_kernel,
        grid=(1,),
        out_shape=jax.ShapeDtypeStruct((load_rows, wide), BF16),
        in_specs=[pl.BlockSpec((length, LANES), lambda i: (0, 2))]
        + [pl.BlockSpec(a.shape, lambda i: (0, 0)) for a in args[1:]],
        out_specs=pl.BlockSpec((load_rows, wide), lambda i: (0, 0)),
    )(*args)
    core_here = (tp % 2).astype(jnp.int32)
    pieces = [(2 * length, LANES)] * 2 + [(length, LANES)] + [(WINDOW, LANES)] * 2
    q_den, q_win, kv_win, give, keep = run(
        rest_kernel, pieces, (core_here.reshape(1), total, gains, cos_w, sin_w, cos_d, sin_d), smem=1
    )
    place = jnp.stack([offset, length * n, core_here]).astype(jnp.int32)
    def dense(blocks, carry, last):
        shape = jax.ShapeDtypeStruct((2 * length, LANES), BF16 if last else F32)
        args = (q_den, *blocks, *carry)
        return pl.pallas_call(
            functools.partial(dense_kernel, not carry, last, len(blocks)),
            out_shape=[shape] if last else [shape, shape],
            in_specs=[pl.BlockSpec(memory_space=pltpu.VMEM)] * len(args),
            out_specs=[pl.BlockSpec(memory_space=pltpu.VMEM)] * (1 if last else 2),
        )(*args)

    own, par = load, swap(load)
    every, owners, carry, used = [load], [me], (), 0
    for d in range(1, half + 1):
        if d == 2:
            own, give, keep, kv_win, q_den, q_win = lax.optimization_barrier((own, give, keep, kv_win, q_den, q_win))
            passed = swap(give)
        if d == 3:
            own, passed = lax.optimization_barrier((own, passed))
            edges = step(jnp.concatenate([keep, passed], axis=0))
        if d == 5:
            own, edges = lax.optimization_barrier((own, edges))
            far_edge = swap(edges[WINDOW:])
        if d == 7:
            (att_win,) = run(
                window_kernel, [(length, LANES)], (place, sink_logit, q_win, edges, kv_win, far_edge), smem=2
            )
            own, att_win = lax.optimization_barrier((own, att_win))
        if d >= 4 and d % 2 == 0:
            own, carry = lax.optimization_barrier((own, carry))
        own = step(own)
        every.append(own)
        owners.append(me - way * d)
        if d < half:
            par = step(par)
            every.append(swap(par))
            owners.append(me + way * d)
        while len(every) - used >= 4 and d < half:
            carry = dense(every[used : used + 4], carry, False)
            used += 4
    (att_den,) = dense(every[used:], carry, True)
    owners = jnp.stack(owners).astype(jnp.int32) % n
    places_out = every
    core, x = tp % 2, tp // 2
    nx = ntp // 2
    share = length // ntp

    def product(which):
        turns = jnp.stack([((x + r) % nx) * 2 + which for r in range(nx)]).astype(jnp.int32)
        (res,) = run(
            out_kernel, [(nx, share, wide * n)], (turns, owners, att_win, att_den, *places_out), smem=2
        )
        return res

    given = lax.ppermute(product(1 - core), "tp", [(i, i ^ 1) for i in range(ntp)])
    kept = product(core)
    sums = [kept[r].astype(F32) + given[r].astype(F32) for r in range(nx)]
    got = {}
    for r in sorted(range(1, nx), key=lambda r: -min(r, nx - r)):
        got[r] = lax.ppermute(sums[r].astype(BF16), "tp", [(i, (i + 2 * r) % ntp) for i in range(ntp)])
    out = sums[0]
    for r in range(1, nx):
        out = out + got[r].astype(F32)
    return out.astype(BF16)


def solution(mesh):
    return jax.shard_map(
        local,
        mesh=mesh,
        in_specs=(
            P(("grp", "sp"), None),
            P(),
            P("sp", "tp"),
            P("sp", "tp"),
            P("sp", "tp"),
            P(),
            P(),
            P("tp"),
            P("sp", "tp"),
            P("sp", "tp"),
            P("sp", "tp"),
            P(),
            P(),
            P("tp", "sp"),
            P("tp", "sp"),
        ),
        out_specs=P(("grp", "sp", "tp"), None),
        check_vma=False,
    )
```

```python
import functools

import jax
import jax.numpy as jnp
from jax import lax
from jax.experimental import pallas as pl
from jax.experimental.pallas import tpu as pltpu
from jax.sharding import PartitionSpec as P

HD = 64
WINDOW = 128
GRID_W = 64
EPS = 1e-06
THETA = 10000.0
LANES = 2 * HD
F32 = jnp.float32
BF16 = jnp.bfloat16


def dotf(a, b):
    return jnp.dot(a, b, preferred_element_type=F32)


def frequencies(width):
    return THETA ** (-jnp.arange(0, width, 2, dtype=F32) / width)


def packed_angles(places):
    line, grid = frequencies(HD), frequencies(HD // 2)
    inverse = jnp.concatenate([line, grid, grid, jnp.zeros((HD,), F32)])
    lane = lax.broadcasted_iota(jnp.int32, (places.shape[0], LANES), 1)
    t = places[:, None]
    at = jnp.where(lane < HD // 2, t, jnp.where(lane < 3 * HD // 4, t // GRID_W, t % GRID_W))
    return at.astype(F32) * inverse[None, :]


def table_kernel(cosine, sine, cos_w, sin_w, cos_d, sin_d):
    lane = lane_index(cosine.shape[0])
    quarter = HD // 4

    def between(x, low, high):
        return jnp.where((lane >= low) & (lane < high), x, 0.0)

    def line(x):
        x = between(x, 0, 2 * quarter)
        x = x + pltpu.roll(x, 2 * quarter, 1)
        return x + pltpu.roll(x, 4 * quarter, 1)

    def grid(x):
        row = pltpu.roll(between(x, 2 * quarter, 3 * quarter), LANES - 2 * quarter, 1)
        col = pltpu.roll(between(x, 3 * quarter, 4 * quarter), LANES - quarter, 1)
        x = row + col
        x = x + pltpu.roll(x, quarter, 1)
        return x + pltpu.roll(x, 4 * quarter, 1)

    cos_w[...] = line(cosine[...])
    cos_d[...] = grid(cosine[...])
    x = line(sine[...])
    sin_w[...] = jnp.where(lane % HD < HD // 2, -x, x)
    x = grid(sine[...])
    sin_d[...] = jnp.where(lane % (HD // 2) < quarter, -x, x)


def join_kernel(dq, wq, dk, dv, wk, wv, out):
    out[:, 0:LANES] = dq[...]
    out[:, LANES : 2 * LANES] = wq[...]
    pair = jnp.concatenate([dk[...], dv[...]], axis=0).astype(F32)
    out[:, 2 * LANES : 3 * LANES] = pair.T.astype(BF16)
    pair = jnp.concatenate([wk[...], wv[...]], axis=0).astype(F32)
    out[:, 3 * LANES : 4 * LANES] = pair.T.astype(BF16)


def lane_index(rows):
    return lax.broadcasted_iota(jnp.int32, (rows, LANES), 1)


def head_norm(x, lane, gain):
    squares = x * x
    low = jnp.sum(jnp.where(lane < HD, squares, 0.0), axis=-1, keepdims=True)
    high = jnp.sum(jnp.where(lane < HD, 0.0, squares), axis=-1, keepdims=True)
    mean = jnp.where(lane < HD, low, high) * (1.0 / HD)
    return x * lax.rsqrt(mean + EPS) * gain


def turn(x, lane, cosine, sine, half):
    up = pltpu.roll(x, LANES - half, 1)
    down = pltpu.roll(x, half, 1)
    return x * cosine + jnp.where(lane % (2 * half) < half, up, down) * sine


def keyed_values(x, lane, gain, cosine, sine, half):
    return jnp.where(lane < HD, turn(head_norm(x, lane, gain), lane, cosine, sine, half), x).astype(BF16)


def load_kernel(acc, gains, cos_d, sin_d, wo_win, wo_den, load):
    rows = acc.shape[0]
    lane = lane_index(rows)
    high, part = wo_win.shape[0], rows // 2
    kv = keyed_values(acc[...], lane, gains[2:3, :], cos_d[...], sin_d[...], HD // 4)
    load[2 * high : 2 * high + part, 0:LANES] = kv[0:part]
    load[2 * high : 2 * high + part, LANES : 2 * LANES] = kv[part:rows]
    load[0:high, :] = wo_win[...]
    load[high : 2 * high, :] = wo_den[...]


def rest_kernel(core, acc, gains, cos_w, sin_w, cos_d, sin_d, q_den, q_win, kv_win, give, keep):
    rows = acc.shape[0]
    lane = lane_index(rows)

    def put_query(out, col, cosine, sine, half):
        normed = head_norm(acc[:, col * LANES : (col + 1) * LANES], lane, gains[col : col + 1, :])
        turned = turn(normed, lane, cosine[...], sine[...], half)
        out[0:rows, :] = jnp.where(lane < HD, turned, 0.0).astype(BF16)
        out[rows : 2 * rows, :] = jnp.where(lane < HD, pltpu.roll(turned, HD, 1), 0.0).astype(BF16)

    kv = keyed_values(acc[:, 3 * LANES :], lane, gains[3:4, :], cos_w[...], sin_w[...], HD // 2)
    kv_win[...] = kv
    first = core[0] == 0
    head, tail = kv[:WINDOW].astype(F32), kv[rows - WINDOW :].astype(F32)
    give[...] = jnp.where(first, head, tail).astype(BF16)
    keep[...] = jnp.where(first, tail, head).astype(BF16)
    put_query(q_den, 0, cos_d, sin_d, HD // 4)
    put_query(q_win, 1, cos_w, sin_w, HD // 2)


def qkt(q, k):
    return lax.dot_general(q, k, (((1,), (1,)), ((), ())), preferred_element_type=F32)


def join_heads(first, second, lane):
    return jnp.where(lane < HD, pltpu.roll(first, HD, 1), second).astype(BF16)


def window_kernel(place, sinks, q, mine, mid, other, out):
    rows = mid.shape[0]
    first = place[2] == 0
    one, two = mine[0:WINDOW, :].astype(F32), other[...].astype(F32)
    low, high = jnp.where(first, one, two).astype(BF16), jnp.where(first, two, one).astype(BF16)
    ext = jnp.concatenate([low, mid[...], high], axis=0)
    span = 3 * WINDOW
    lane = lane_index(WINDOW)
    row = lax.broadcasted_iota(jnp.int32, (WINDOW, span), 0)
    col = lax.broadcasted_iota(jnp.int32, (WINDOW, span), 1)
    near = (col - row >= 0) & (col - row <= 2 * WINDOW)
    scores, valid, floor, near_kv = [], [], [], []
    for n in range(rows // WINDOW):
        kv = ext[n * WINDOW : n * WINDOW + span, :]
        near_kv.append(kv)
        key_pos = place[0] + (n - 1) * WINDOW + col
        for h in range(2):
            scores.append(qkt(q[h * rows + n * WINDOW : h * rows + (n + 1) * WINDOW, :], kv))
            valid.append(near & (key_pos >= 0) & (key_pos < place[1]))
            floor.append(jnp.full((WINDOW, 1), sinks[h], F32))
    floor = jnp.concatenate(floor, axis=0)
    s = jnp.concatenate([jnp.where(v, x * HD ** (-0.5), -jnp.inf) for v, x in zip(valid, scores)], axis=0)
    top = jnp.maximum(jnp.max(s, axis=-1, keepdims=True), floor)
    e = jnp.exp(s - top)
    weights = e / (jnp.sum(e, axis=-1, keepdims=True) + jnp.exp(floor - top))
    weights = weights.astype(BF16)
    for n, kv in enumerate(near_kv):
        base = 2 * n * WINDOW
        first_head = dotf(weights[base : base + WINDOW], kv)
        second_head = dotf(weights[base + WINDOW : base + 2 * WINDOW], kv)
        out[n * WINDOW : (n + 1) * WINDOW, :] = join_heads(first_head, second_head, lane)


def dense_kernel(first, last, count, *refs):
    q, blocks, rest = refs[0], refs[1 : 1 + count], refs[1 + count :]
    carry, outs = ((), rest) if first else (rest[:2], rest[2:])
    scale = HD ** (-0.5) * 1.4426950408889634
    half = blocks[0].shape[0] - 2 * LANES
    rows = q.shape[0] // 2

    def keys(ref):
        block = ref[ref.shape[0] - half :, :]
        return [block[:, :LANES], block[:, LANES:]]

    for h in range(2):
        at = slice(h * rows, (h + 1) * rows)
        query = q[at, :]
        acc, top = (None, None) if first else (carry[0][at, :], carry[1][at, 0:1])
        for k in range(0, count, 4):
            kv = jnp.concatenate([x for ref in blocks[k : k + 4] for x in keys(ref)], axis=0)
            wide = lax.broadcasted_iota(jnp.int32, kv.shape, 1)
            values = jnp.where(wide < HD, jnp.ones_like(kv), kv)
            s = qkt(query, kv)
            here = jnp.max(s, axis=-1, keepdims=True)
            new = here if top is None else jnp.maximum(top, here)
            p = jnp.exp2((s - new) * scale).astype(BF16)
            part = dotf(p, values)
            acc = part if top is None else acc * jnp.exp2((top - new) * scale) + part
            top = new
        if last:
            outs[0][at, :] = (acc / pltpu.roll(acc, HD, 1)).astype(BF16)
        else:
            outs[0][at, :] = acc
            outs[1][at, :] = jnp.broadcast_to(top, acc.shape)


def out_kernel(turns, owners, att_win, att_den, *refs):
    blocks, out = refs[:-1], refs[-1]
    parts, share, _ = out.shape
    rows = att_win.shape[0]
    lane = lane_index(share)
    pieces = []
    for r in range(parts):
        at = pl.multiple_of(turns[r] * share, 16)
        low = att_den[pl.ds(at, share), :].astype(F32)
        high = att_den[pl.ds(rows + at, share), :].astype(F32)
        pieces.append(jnp.concatenate([att_win[pl.ds(at, share), :], join_heads(low, high, lane)], axis=1))
    att = jnp.concatenate(pieces, axis=0)
    for i, block in enumerate(blocks):
        width = block.shape[1]
        res = dotf(att, block[0:width, :]).astype(BF16)
        cols = pl.ds(pl.multiple_of(owners[i] * width, width), width)
        for r in range(parts):
            out[r, :, cols] = res[r * share : (r + 1) * share, :]


def run(kernel, outs, args, smem=0, dtype=BF16, **more):
    specs = [pl.BlockSpec(memory_space=pltpu.SMEM)] * smem + [pl.BlockSpec(memory_space=pltpu.VMEM)] * (len(args) - smem)
    return pl.pallas_call(
        kernel,
        out_shape=[jax.ShapeDtypeStruct(s, dtype) for s in outs],
        in_specs=specs,
        **more,
        out_specs=[pl.BlockSpec(memory_space=pltpu.VMEM)] * len(outs),
    )(*args)


def swap(x):
    return lax.ppermute(x, "tp", [(i, i ^ 1) for i in range(lax.axis_size("tp"))])


def step(x):
    n, t = lax.axis_size("sp"), lax.axis_size("tp")
    pairs = [(s * t + c, (s + 1 - 2 * (c % 2)) % n * t + c) for s in range(n) for c in range(t)]
    return lax.ppermute(x, ("sp", "tp"), pairs)


def local(
    tokens_in,
    norm_gain,
    window_query,
    window_key,
    window_value,
    window_query_gain,
    window_key_gain,
    sink_logit,
    dense_query,
    dense_key,
    dense_value,
    dense_query_gain,
    dense_key_gain,
    window_out,
    dense_out,
):
    length = tokens_in.shape[0]
    n = lax.axis_size("sp")
    half = n // 2
    me = lax.axis_index("sp")
    tp = lax.axis_index("tp")
    ntp = lax.axis_size("tp")
    depth = window_query.shape[0]
    way = 1 - 2 * (tp % 2)

    (block,) = run(
        join_kernel,
        [(depth, 4 * LANES)],
        (dense_query, window_query, dense_key.T, dense_value.T, window_key.T, window_value.T),
    )
    inputs = tokens_in.astype(F32)
    inverse = lax.rsqrt(jnp.mean(inputs * inputs, axis=-1, keepdims=True) + EPS)

    def product_in(owner, weights):
        return dotf(lax.dynamic_slice_in_dim(normed, (owner % n) * depth, depth, axis=1), weights)

    own = block
    par = swap(block)
    offset = me * length
    for d in range(1, half + 1):
        own = step(own)
        if d < half:
            par = step(par)
            if d == 1:
                inverse, par = lax.optimization_barrier((inverse, par))
                normed = (inputs * inverse * norm_gain).astype(BF16)
                total = product_in(me, block)
            total = total + product_in(me + way * d, swap(par))
        if d == 4:
            offset, own = lax.optimization_barrier((offset, own))
        total = total + product_in(me - way * d, own)

    angles = packed_angles(offset + jnp.arange(length, dtype=jnp.int32))
    cos_w, sin_w, cos_d, sin_d = run(
        table_kernel, [(length, LANES)] * 4, (jnp.cos(angles), jnp.sin(angles)), dtype=F32
    )
    gains = jnp.stack(
        [jnp.tile(g, 2) for g in (dense_query_gain, window_query_gain, dense_key_gain, window_key_gain)]
    )
    wide = window_out.shape[1]
    load_rows = 2 * window_out.shape[0] + length // 2
    args = (total, gains, cos_d, sin_d, window_out, dense_out)
    load = pl.pallas_call(
        load_kernel,
        grid=(1,),
        out_shape=jax.ShapeDtypeStruct((load_rows, wide), BF16),
        in_specs=[pl.BlockSpec((length, LANES), lambda i: (0, 2))]
        + [pl.BlockSpec(a.shape, lambda i: (0, 0)) for a in args[1:]],
        out_specs=pl.BlockSpec((load_rows, wide), lambda i: (0, 0)),
    )(*args)
    core_here = (tp % 2).astype(jnp.int32)
    pieces = [(2 * length, LANES)] * 2 + [(length, LANES)] + [(WINDOW, LANES)] * 2
    q_den, q_win, kv_win, give, keep = run(
        rest_kernel, pieces, (core_here.reshape(1), total, gains, cos_w, sin_w, cos_d, sin_d), smem=1
    )
    place = jnp.stack([offset, length * n, core_here]).astype(jnp.int32)
    def dense(blocks, carry, last):
        shape = jax.ShapeDtypeStruct((2 * length, LANES), BF16 if last else F32)
        args = (q_den, *blocks, *carry)
        return pl.pallas_call(
            functools.partial(dense_kernel, not carry, last, len(blocks)),
            out_shape=[shape] if last else [shape, shape],
            in_specs=[pl.BlockSpec(memory_space=pltpu.VMEM)] * len(args),
            out_specs=[pl.BlockSpec(memory_space=pltpu.VMEM)] * (1 if last else 2),
        )(*args)

    own, par = load, swap(load)
    every, owners, carry, used = [load], [me], (), 0
    for d in range(1, half + 1):
        if d == 2:
            own, give, keep, kv_win, q_den, q_win = lax.optimization_barrier((own, give, keep, kv_win, q_den, q_win))
            passed = swap(give)
        if d == 3:
            own, passed = lax.optimization_barrier((own, passed))
            edges = step(jnp.concatenate([keep, passed], axis=0))
        if d == 5:
            own, edges = lax.optimization_barrier((own, edges))
            far_edge = swap(edges[WINDOW:])
        if d == 7:
            (att_win,) = run(
                window_kernel, [(length, LANES)], (place, sink_logit, q_win, edges, kv_win, far_edge), smem=2
            )
            own, att_win = lax.optimization_barrier((own, att_win))
        if d >= 4 and d % 2 == 0:
            own, carry = lax.optimization_barrier((own, carry))
        own = step(own)
        every.append(own)
        owners.append(me - way * d)
        if d < half:
            par = step(par)
            every.append(swap(par))
            owners.append(me + way * d)
        while len(every) - used >= 4 and d < half:
            carry = dense(every[used : used + 4], carry, False)
            used += 4
    (att_den,) = dense(every[used:], carry, True)
    owners = jnp.stack(owners).astype(jnp.int32) % n
    places_out = every
    core, x = tp % 2, tp // 2
    nx = ntp // 2
    share = length // ntp

    def chip_sums(att, turns):
        def product(which):
            at = jnp.stack([((x + r) % nx) * 2 + which for r in turns]).astype(jnp.int32)
            shape = (len(turns), share, wide * n)
            (res,) = run(out_kernel, [shape], (at, owners, att_win, att, *places_out), smem=2)
            return res

        given = swap(product(1 - core))
        kept = product(core)
        return [kept[i].astype(F32) + given[i].astype(F32) for i in range(len(turns))]

    def sent(value, r):
        return lax.ppermute(value.astype(BF16), "tp", [(i, (i + 2 * r) % ntp) for i in range(ntp)])

    far = nx // 2
    (far_sum,) = chip_sums(att_den, [far])
    far_sum, att_den = lax.optimization_barrier((far_sum.astype(BF16), att_den))
    got = [sent(far_sum, far)]
    near_turns = [r for r in range(1, nx) if r != far]
    sums = chip_sums(att_den, near_turns + [0])
    got += [sent(value, r) for value, r in zip(sums, near_turns)]
    out = sums[-1]
    for value in got:
        out = out + value.astype(F32)
    return out.astype(BF16)


def solution(mesh):
    return jax.shard_map(
        local,
        mesh=mesh,
        in_specs=(
            P(("grp", "sp"), None),
            P(),
            P("sp", "tp"),
            P("sp", "tp"),
            P("sp", "tp"),
            P(),
            P(),
            P("tp"),
            P("sp", "tp"),
            P("sp", "tp"),
            P("sp", "tp"),
            P(),
            P(),
            P("tp", "sp"),
            P("tp", "sp"),
        ),
        out_specs=P(("grp", "sp", "tp"), None),
        check_vma=False,
    )
```
